32 devices in a mesh: sp: 16 (over z, y, x), tp: 2 (over core).
Axes of the slice: x: 2, y: 2, z: 4, core: 2. Of those that a mesh axis runs over, the one named last changes fastest.
Arguments:
- resid: bfloat16 [2048, 2048], P('sp', 'tp'), may hold values from -6 to 6
- qa_nope: bfloat16 [2048, 1024], P('sp', 'tp'), may hold values from -6 to 6
- qb_nope: bfloat16 [2048, 1024], P('sp', 'tp'), may hold values from -6 to 6
- qa_rope: bfloat16 [2048, 512], P('sp', 'tp'), may hold values from -360 to 360
- qb_rope: bfloat16 [2048, 256], P('sp', 'tp'), may hold values from -360 to 360
- latent: bfloat16 [2048, 256], P('sp'), may hold values from -6 to 6
- key_rope: bfloat16 [2048, 32], P('sp'), may hold values from -4 to 4
- lat_gain: float32 [256], replicated, may hold values from 0.1 to 1.9
- wa_key: bfloat16 [256, 1024], P(None, 'tp'), may hold values from -0.375 to 0.375
- wa_val: bfloat16 [256, 1024], P(None, 'tp'), may hold values from -0.75 to 0.75
- wb_key: bfloat16 [256, 1024], P(None, 'tp'), may hold values from -0.375 to 0.375
- wb_val: bfloat16 [256, 1024], P(None, 'tp'), may hold values from -0.75 to 0.75
- gain_a: float32 [1024], P('tp'), may hold values from 0.1 to 1.9
- gain_b: float32 [1024], P('tp'), may hold values from 0.1 to 1.9
- wa_out: bfloat16 [1024, 2048], P('tp'), may hold values from -0.125 to 0.125
- wb_out: bfloat16 [1024, 2048], P('tp'), may hold values from -0.125 to 0.125
- norm1_gain: float32 [2048], replicated, may hold values from 0.1 to 1.9
- ffn_gate: bfloat16 [2048, 5632], P('sp', 'tp'), may hold values from -0.125 to 0.125
- ffn_val: bfloat16 [2048, 5632], P('sp', 'tp'), may hold values from -0.125 to 0.125
- conv_gate: float32 [3, 5632], P(None, 'tp'), may hold values from -3 to 3
- conv_val: float32 [3, 5632], P(None, 'tp'), may hold values from -3 to 3
- ffn_down: bfloat16 [5632, 2048], P('tp'), may hold values from -0.078125 to 0.078125
- norm2_gain: float32 [2048], P('tp'), may hold values from 0.1 to 1.9
Outputs:
- layer_out: bfloat16 [2048, 2048], P('sp', 'tp')
The draws below stay inside these ranges and needn't reach their ends.
All inputs are finite; a program needn't handle non-finite values.
Results may differ from the reference program's by a relative error of at most 0.017.
Values may be sent and summed in bfloat16 or wider, within the bound.
A program may use at most 128 MiB of HBM per device.

```python
import math
import jax
import jax.numpy as jnp
from jax import lax

D = 2048
HA = 16
DA = 64
HB = 8
DB = 128
DR = 32
LAT = 256
FF = 5632
KC = 3
TOKENS = 2048


def drawn(key):
    base = jnp.clip(jax.random.normal(jax.random.fold_in(key, 101), (TOKENS, DR), jnp.float32), -4.0, 4.0)
    return base


def draw_key_rope(key, part):
    base = drawn(key)
    return base.astype(jnp.bfloat16)


def draw_qa_rope(key, part):
    noise = jnp.clip(jax.random.normal(jax.random.fold_in(key, 104), (TOKENS, HA * DR), jnp.float32), -6.0, 6.0)
    return noise.astype(jnp.bfloat16)


def draw_qb_rope(key, part):
    noise = jnp.clip(jax.random.normal(jax.random.fold_in(key, 105), (TOKENS, HB * DR), jnp.float32), -6.0, 6.0)
    return noise.astype(jnp.bfloat16)


def rising_value(key, heads, width):
    noise = jnp.clip(jax.random.normal(key, (LAT, heads * width), jnp.float32), -6.0, 6.0) * LAT ** (-0.5)
    head_index = (jnp.arange(heads * width) // width).astype(jnp.float32)
    factor = 0.5 * 4.0 ** (head_index / (heads - 1))
    return (noise * factor[None, :]).astype(jnp.bfloat16)


def draw_wa_val(key, part):
    return rising_value(jax.random.fold_in(key, 201), HA, DA)


def draw_wb_val(key, part):
    return rising_value(jax.random.fold_in(key, 202), HB, DB)


def levels(stream_key, extent, shards, least, top_value):
    loudness = 1.0
    for dim, shards_of in shards:
        draws = jax.random.uniform(jax.random.fold_in(jax.random.fold_in(stream_key, 6), dim), (shards_of,), jnp.float32, least / len(shards), top_value / len(shards))
        loudness = loudness * jnp.repeat(jnp.exp(draws), extent[dim] // shards_of).reshape((-1,) + (1,) * (len(extent) - 1 - dim))
    return loudness


def gaussian(key, shape, scale, bound, cuts=(), kind=jnp.bfloat16):
    result = scale * jax.random.normal(key, shape, jnp.float32)
    if cuts:
        result = result * levels(key, shape, cuts, -0.22, 0.18)
    return jnp.clip(result, -bound, bound).astype(kind)


def setup_inputs(seed: int = 0) -> dict:
    key_list = jax.random.split(jax.random.key(seed), 24)
    resid = gaussian(key_list[0], (TOKENS, D), 1.0, 6.0, ((0, 16), (1, 2)))
    qa_nope = gaussian(key_list[1], (TOKENS, HA * DA), 1.0, 6.0, ((0, 16), (1, 2)))
    qb_nope = gaussian(key_list[2], (TOKENS, HB * DB), 1.0, 6.0, ((0, 16), (1, 2)))
    qa_rope = draw_qa_rope(jax.random.fold_in(key_list[23], 71), 0)
    qb_rope = draw_qb_rope(jax.random.fold_in(key_list[23], 71), 0)
    latent = gaussian(key_list[5], (TOKENS, LAT), 1.0, 6.0, ((0, 16),))
    key_rope = draw_key_rope(jax.random.fold_in(key_list[23], 71), 0)
    lat_gain = jnp.clip(1.0 + 0.18 * jax.random.normal(key_list[7], (LAT,), jnp.float32), 0.1, 1.9)
    wa_key = gaussian(key_list[8], (LAT, HA * DA), LAT ** -0.5, 0.375, ((1, 2),))
    wa_val = draw_wa_val(jax.random.fold_in(key_list[23], 71), 0)
    wb_key = gaussian(key_list[10], (LAT, HB * DB), LAT ** -0.5, 0.375, ((1, 2),))
    wb_val = draw_wb_val(jax.random.fold_in(key_list[23], 71), 0)
    gain_a = jnp.clip(1.0 + 0.18 * jax.random.normal(key_list[12], (HA * DA,), jnp.float32), 0.1, 1.9)
    gain_b = jnp.clip(1.0 + 0.18 * jax.random.normal(key_list[13], (HB * DB,), jnp.float32), 0.1, 1.9)
    wa_out = gaussian(key_list[14], (HA * DA, D), (HA * DA + HB * DB) ** -0.5, 0.125, ((0, 2),))
    wb_out = gaussian(key_list[15], (HB * DB, D), (HA * DA + HB * DB) ** -0.5, 0.125, ((0, 2),))
    norm1_gain = jnp.clip(1.0 + 0.18 * jax.random.normal(key_list[16], (D,), jnp.float32), 0.1, 1.9)
    ffn_gate = gaussian(key_list[17], (D, FF), D ** -0.5, 0.125, ((0, 16), (1, 2)))
    ffn_val = gaussian(key_list[18], (D, FF), D ** -0.5, 0.125, ((0, 16), (1, 2)))
    conv_gate = gaussian(key_list[19], (KC, FF), 0.577, 3.0, ((1, 2),), jnp.float32)
    conv_val = gaussian(key_list[20], (KC, FF), 0.577, 3.0, ((1, 2),), jnp.float32)
    ffn_down = gaussian(key_list[21], (FF, D), FF ** -0.5, 0.078125, ((0, 2),))
    norm2_gain = jnp.clip(1.0 + 0.18 * jax.random.normal(key_list[22], (D,), jnp.float32), 0.1, 1.9)
    return dict(resid=resid, qa_nope=qa_nope, qb_nope=qb_nope, qa_rope=qa_rope, qb_rope=qb_rope, latent=latent, key_rope=key_rope, lat_gain=lat_gain, wa_key=wa_key, wa_val=wa_val, wb_key=wb_key, wb_val=wb_val, gain_a=gain_a, gain_b=gain_b, wa_out=wa_out, wb_out=wb_out, norm1_gain=norm1_gain, ffn_gate=ffn_gate, ffn_val=ffn_val, conv_gate=conv_gate, conv_val=conv_val, ffn_down=ffn_down, norm2_gain=norm2_gain)


THETA = 10000.0
EPS_RMS = 1e-06
EPS_NORM = 1e-05
ALPHA = 2.0 ** 0.25

def stored(values):
    return lax.optimization_barrier(values.astype(jnp.bfloat16))

def rotary(values, positions):
    half = values.shape[-1] // 2
    freq = THETA ** (-jnp.arange(half, dtype=jnp.float32) * 2.0 / values.shape[-1])
    angle = positions.astype(jnp.float32)[:, None] * freq[None, :]
    if values.ndim == 3:
        angle = angle[:, None, :]
    cosine = jnp.cos(angle)
    sine = jnp.sin(angle)
    first = values[..., :half]
    second = values[..., half:]
    return jnp.concatenate([first * cosine - second * sine, second * cosine + first * sine], axis=-1)

def rms_scale(values, gain):
    wide = values.astype(jnp.float32)
    return wide * lax.rsqrt(lax.optimization_barrier(jnp.mean(wide * wide, axis=-1, keepdims=True)) + EPS_RMS) * gain.astype(jnp.float32)

def layer_norm(values, gain):
    center = lax.optimization_barrier(jnp.mean(values, axis=-1, keepdims=True))
    shifted = values - center
    spread = lax.optimization_barrier(jnp.mean(shifted * shifted, axis=-1, keepdims=True))
    return shifted * lax.rsqrt(spread + EPS_NORM) * gain.astype(jnp.float32)

def attend(query, q_rot, keys, k_rot, vals):
    total_rows, heads, width = query.shape
    scale = (width + k_rot.shape[-1]) ** (-0.5)
    block = math.gcd(512, total_rows)
    key_pos = jnp.arange(total_rows)
    keys_wide = keys.astype(jnp.float32)
    rot_wide = k_rot.astype(jnp.float32)
    vals_wide = vals.astype(jnp.float32)

    def one_block(index):
        start = index * block
        q_part = lax.dynamic_slice_in_dim(query, start, block, 0).astype(jnp.float32)
        r_part = lax.dynamic_slice_in_dim(q_rot, start, block, 0).astype(jnp.float32)
        scores = jnp.einsum('qhd,khd->hqk', q_part, keys_wide) + jnp.einsum('qhr,kr->hqk', r_part, rot_wide)
        scores = scores * scale
        q_pos = start + jnp.arange(block)
        allowed = key_pos[None, :] <= q_pos[:, None]
        scores = jnp.where(allowed[None], scores, -jnp.inf)
        top = lax.optimization_barrier(jnp.max(scores, axis=-1, keepdims=True))
        weights = jnp.exp(scores - top)
        total = lax.optimization_barrier(jnp.sum(weights, axis=-1))
        rounded = stored(weights).astype(jnp.float32)
        mixed = jnp.einsum('hqk,khd->qhd', rounded, vals_wide)
        return mixed / jnp.transpose(total)[:, :, None]
    out = lax.map(one_block, jnp.arange(total_rows // block)).reshape(total_rows, heads * width)
    return out

def causal_conv(values, taps):
    count = values.shape[0]
    padded = jnp.pad(values.astype(jnp.float32), ((KC - 1, 0), (0, 0)))
    total = jnp.zeros(values.shape, jnp.float32)
    for tap in range(KC):
        total = total + taps[tap].astype(jnp.float32) * padded[tap:tap + count]
    return total

def reference(resid, qa_nope, qb_nope, qa_rope, qb_rope, latent, key_rope, lat_gain, wa_key, wa_val, wb_key, wb_val, gain_a, gain_b, wa_out, wb_out, norm1_gain, ffn_gate, ffn_val, conv_gate, conv_val, ffn_down, norm2_gain):
    positions = jnp.arange(TOKENS)
    lat_n = stored(rms_scale(latent, lat_gain))
    k_rot = stored(rotary(key_rope.astype(jnp.float32), positions))

    def group(q_nope, q_rope, w_key, w_val, width):
        heads = q_nope.shape[1] // width
        q_rot = stored(rotary(q_rope.astype(jnp.float32).reshape(TOKENS, heads, DR), positions))
        keys = stored(jnp.dot(lat_n, w_key, preferred_element_type=jnp.float32)).reshape(TOKENS, heads, width)
        vals = stored(jnp.dot(lat_n, w_val, preferred_element_type=jnp.float32)).reshape(TOKENS, heads, width)
        return attend(q_nope.reshape(TOKENS, heads, width), q_rot, keys, k_rot, vals)
    raw_a = group(qa_nope, qa_rope, wa_key, wa_val, DA)
    raw_b = group(qb_nope, qb_rope, wb_key, wb_val, DB)
    energy = lax.optimization_barrier(jnp.sum(raw_a * raw_a, axis=-1)) + lax.optimization_barrier(jnp.sum(raw_b * raw_b, axis=-1))
    factor = lax.rsqrt(energy / (HA * DA + HB * DB) + EPS_RMS)[:, None]
    part_a = stored(raw_a * factor * gain_a.astype(jnp.float32))
    part_b = stored(raw_b * factor * gain_b.astype(jnp.float32))
    mix = jnp.dot(part_a, wa_out, preferred_element_type=jnp.float32) + jnp.dot(part_b, wb_out, preferred_element_type=jnp.float32)
    first = stored(layer_norm(ALPHA * resid.astype(jnp.float32) + mix, norm1_gain))
    gate_up = stored(jnp.dot(first, ffn_gate, preferred_element_type=jnp.float32))
    val_up = stored(jnp.dot(first, ffn_val, preferred_element_type=jnp.float32))
    gate_c = causal_conv(gate_up, conv_gate)
    val_c = causal_conv(val_up, conv_val)
    hidden = stored(jax.nn.silu(gate_c) * val_c)
    down = jnp.dot(hidden, ffn_down, preferred_element_type=jnp.float32)
    return layer_norm(ALPHA * first.astype(jnp.float32) + down, norm2_gain).astype(jnp.bfloat16)
```

```python
import functools

import jax
import jax.numpy as jnp
from jax import lax
from jax.experimental import pallas as pl
from jax.experimental.pallas import tpu as pltpu
from jax.sharding import PartitionSpec as P

D = 2048
HA = 16
DA = 64
HB = 8
DB = 128
DR = 32
KC = 3


THETA = 10000.0
EPS_RMS = 1e-06
EPS_NORM = 1e-05
ALPHA = 2.0**0.25


def passed_along(value, axis, steps):
    count = lax.axis_size(axis)
    leading, last = (max(0, -steps), min(count, count - steps))
    return lax.ppermute(value, axis, [(source, source + steps) for source in range(leading, last)])


def rotary(values, positions):
    half = values.shape[-1] // 2
    freq = THETA ** (-jnp.arange(half, dtype=jnp.float32) * 2.0 / values.shape[-1])
    angle = positions.astype(jnp.float32)[:, None] * freq[None, :]
    if values.ndim == 3:
        angle = angle[:, None, :]
    cosine = jnp.cos(angle)
    sine = jnp.sin(angle)
    first = values[..., :half]
    second = values[..., half:]
    return jnp.concatenate(
        [first * cosine - second * sine, second * cosine + first * sine], axis=-1
    )


def rms_scale(values, gain):
    wide = values.astype(jnp.float32)
    return wide * lax.rsqrt(jnp.mean(wide * wide, axis=-1, keepdims=True) + EPS_RMS) * gain


def finish_norm(values, sums, gain, width):
    center = sums[0] / width
    spread = sums[1] / width - center * center
    return (values - center[:, None]) * lax.rsqrt(spread + EPS_NORM)[:, None] * gain


def start_carry(count, heads, width):
    return (
        jnp.full((heads, count), -1e30, jnp.float32),
        jnp.zeros((heads, count), jnp.float32),
        jnp.zeros((count, heads, width), jnp.float32),
    )


def divide_total(carry):
    mixed = carry[2] / jnp.transpose(carry[1])[:, :, None]
    return mixed.reshape(mixed.shape[0], mixed.shape[1] * mixed.shape[2])


def causal_taps(extended, taps, count):
    total = jnp.zeros((count, extended.shape[1]), jnp.float32)
    for tap in range(KC):
        total = total + taps[tap] * extended[tap : tap + count].astype(jnp.float32)
    return total


BF = jnp.bfloat16
LANES = 128
MESH = pl.DeviceIdType.MESH


def greet(n, tp):
    me, core = lax.axis_index("sp"), lax.axis_index("tp")
    barrier = pltpu.get_barrier_semaphore()
    for step in range(1, n):
        pl.semaphore_signal(
            barrier, inc=1, device_id=(lax.rem(me + step, n), core), device_id_type=MESH
        )
    pl.semaphore_signal(barrier, inc=1, device_id=(me, 1 - core), device_id_type=MESH)
    pl.semaphore_wait(barrier, n)


def send(src, dst, send_sem, recv_sem, sp, core):
    return pltpu.make_async_remote_copy(
        src_ref=src,
        dst_ref=dst,
        send_sem=send_sem,
        recv_sem=recv_sem,
        device_id=(sp, core),
        device_id_type=MESH,
    )


def spread_kernel(
    n, lat_ref, weight_ref, lats_ref, weights_ref, own_sem, lat_s, lat_r, share_s, share_r, w_s, w_r
):
    me, core = lax.axis_index("sp"), lax.axis_index("tp")
    cols = weights_ref.shape[1]
    rows = weight_ref.shape[2]

    def piece(chip):
        return weight_ref.at[:, pl.ds(pl.multiple_of(chip * cols, 16), cols), :]

    place = weights_ref.at[:, :, pl.ds(pl.multiple_of(me * rows, rows), rows)]
    own_w = pltpu.make_async_copy(piece(me), place, own_sem.at[0])
    own_l = pltpu.make_async_copy(lat_ref, lats_ref.at[me], own_sem.at[1])
    own_w.start()
    own_l.start()
    greet(n, 2)
    lat_copies, w_copies = [], []
    for step in range(1, n):
        to = lax.rem(me + step, n)
        copy = send(
            lat_ref.at[core], lats_ref.at[me, core], lat_s.at[step], lat_r.at[step], to, core
        )
        copy.start()
        lat_copies.append(copy)
    for step in range(1, n):
        to = lax.rem(me + step, n)
        copy = send(piece(to), place, w_s.at[step], w_r.at[step], to, core)
        copy.start()
        w_copies.append(copy)
    shares = []
    for step in range(1, n):
        source = lax.rem(me + n - step, n)
        lat_copies[step - 1].wait_recv()
        block = lats_ref.at[source, core]
        copy = send(block, block, share_s.at[step], share_r.at[step], me, 1 - core)
        copy.start()
        shares.append(copy)
    for copy in shares:
        copy.wait()
    for copy in lat_copies:
        copy.wait_send()
    for copy in w_copies:
        copy.wait()
    own_w.wait()
    own_l.wait()


def feed_kernel(
    n,
    part_ref,
    energy_ref,
    resid_ref,
    gain1_ref,
    weight_ref,
    taps_ref,
    down_hbm,
    gain2_ref,
    out_ref,
    part_in,
    energy_in,
    resid_in,
    first_ref,
    full,
    ups,
    hidden_out,
    hidden_in,
    down_ref,
    sums_out,
    sums_in,
    pre_ref,
    down_sem,
    pair_s,
    pair_r,
    z_s,
    z_r,
    x_s,
    x_r,
    y_s,
    y_r,
    dx_s,
    dx_r,
    dy_s,
    dy_r,
    p_s,
    p_r,
    h_s,
    h_r,
):
    me, core = lax.axis_index("sp"), lax.axis_index("tp")
    depth = n // 4
    zi, yi, xi = me // 4, lax.rem(me // 2, 2), lax.rem(me, 2)
    x_peer, y_peer = me + 1 - 2 * xi, me + 2 - 4 * yi
    x_off, y_off = lax.rem(x_peer, 4), lax.rem(y_peer, 4)
    own_off = lax.rem(me, 4)
    diag_off = 3 - own_off
    half_rows = full.shape[2]
    quarter = half_rows // 2
    rows = 2 * half_rows
    columns = resid_ref.shape[1]
    width = part_ref.shape[1]
    cols = hidden_in.shape[1]

    load_down = pltpu.make_async_copy(down_hbm, down_ref, down_sem)
    load_down.start()
    greet(n, 2)
    pair = [
        send(part_ref, part_in, pair_s.at[0], pair_r.at[0], me, 1 - core),
        send(energy_ref, energy_in, pair_s.at[1], pair_r.at[1], me, 1 - core),
        send(resid_ref, resid_in, pair_s.at[2], pair_r.at[2], me, 1 - core),
    ]
    for copy in pair:
        copy.start()
    for copy in pair:
        copy.wait()
    low = (core == 0).astype(jnp.float32)
    mine = resid_ref[...].astype(jnp.float32)
    other = resid_in[...].astype(jnp.float32)
    resid = jnp.concatenate(
        [mine * low + other * (1.0 - low), other * low + mine * (1.0 - low)], axis=1
    )
    energy = (energy_ref[...] + energy_in[...])[:, :1]
    factor = lax.rsqrt(energy / (HA * DA + HB * DB) + EPS_RMS)
    mix = (part_ref[...].astype(jnp.float32) + part_in[...].astype(jnp.float32)) * factor
    pre = ALPHA * resid + mix
    shifted = pre - jnp.mean(pre, axis=1, keepdims=True)
    spread = jnp.mean(shifted * shifted, axis=1, keepdims=True)
    first = (shifted * lax.rsqrt(spread + EPS_NORM) * gain1_ref[...]).astype(BF)
    first_ref[...] = first.reshape(2, half_rows, width)
    full[me] = first.reshape(2, half_rows, width)

    if depth == 4:
        order = [zi, zi + 1 - 2 * lax.rem(zi, 2), 3 - zi, lax.rem(zi + 2, 4)]
        targets = order
    else:
        order = [lax.rem(zi + d, depth) for d in range(depth)]
        targets = [lax.rem(zi + depth - d, depth) for d in range(depth)]

    def line_copy(d):
        return send(
            first_ref.at[core],
            full.at[me, core],
            z_s.at[d],
            z_r.at[d],
            targets[d] * 4 + own_off,
            core,
        )

    def share(block):
        ref = full.at[block, core]
        return send(ref, ref, p_s.at[block], p_r.at[block], me, 1 - core)

    def across(d, x_way):
        block = order[d] * 4 + own_off
        ref = full.at[block, core]
        src = first_ref.at[core] if d == 0 else ref
        if x_way:
            return send(src, ref, x_s.at[d], x_r.at[d], x_peer, core)
        return send(src, ref, y_s.at[d], y_r.at[d], y_peer, core)

    def corner(d, x_way):
        if x_way:
            ref = full.at[order[d] * 4 + y_off, core, pl.ds(0, quarter)]
            return send(ref, ref, dx_s.at[d], dx_r.at[d], x_peer, core)
        ref = full.at[order[d] * 4 + x_off, core, pl.ds(quarter, quarter)]
        return send(ref, ref, dy_s.at[d], dy_r.at[d], y_peer, core)

    lines = [line_copy(d) for d in range(1, depth)]
    started = []

    def go(copy):
        copy.start()
        started.append(copy)

    def stage_a(d):
        if d > 0:
            lines[d - 1].wait_recv()
        go(across(d, True))
        go(across(d, False))
        if d == 0:
            for copy in lines:
                copy.start()
        else:
            go(share(order[d] * 4 + own_off))

    def stage_b(d):
        across(d, True).wait_recv()
        go(corner(d, False))
        go(share(order[d] * 4 + x_off))
        across(d, False).wait_recv()
        go(corner(d, True))
        go(share(order[d] * 4 + y_off))

    def stage_c(d):
        corner(d, True).wait_recv()
        corner(d, False).wait_recv()
        go(share(order[d] * 4 + diag_off))

    def stage_d(d):
        for off in (own_off, x_off, y_off, diag_off):
            if d == 0 and off is own_off:
                continue
            share(order[d] * 4 + off).wait_recv()
        base = order[d] * 4

        def one(step, carry):
            block = base + step
            tokens = full[block].reshape(rows, width)
            up = lax.dot_general(
                weight_ref[...],
                tokens,
                (((1,), (1,)), ((), ())),
                preferred_element_type=jnp.float32,
            )
            ups[block] = up.astype(BF)
            return carry

        lax.fori_loop(0, 4, one, 0)

    for tick in range(depth + 3):
        for stage, lag in ((stage_a, 0), (stage_b, 1), (stage_c, 2), (stage_d, 3)):
            if 0 <= tick - lag < depth:
                stage(tick - lag)

    lane = lax.broadcasted_iota(jnp.int32, (2 * cols, rows), 1)

    def hidden_copy(block):
        return send(
            hidden_out.at[block], hidden_in.at[me], h_s.at[block], h_r.at[me], block, core
        )

    def convolve(block, before):
        current = ups[block].astype(jnp.float32)
        total = taps_ref[:, KC - 1 : KC] * current
        for back in range(1, KC):
            moved = jnp.where(
                lane < back, pltpu.roll(before, back, 1), pltpu.roll(current, back, 1)
            )
            total = total + taps_ref[:, KC - 1 - back : KC - back] * moved
        gate, val = total[:cols], total[cols:]
        hidden = gate / (1.0 + jnp.exp(-gate)) * val
        hidden_out[block] = hidden.astype(BF)

        @pl.when(block == me)
        def _():
            hidden_in[block] = hidden.astype(BF)

        @pl.when((block > 0) & (block - 1 != me))
        def _():
            hidden_copy(block - 1).start()

        return current

    lax.fori_loop(0, n, convolve, jnp.zeros((2 * cols, rows), jnp.float32))

    @pl.when(me != n - 1)
    def _():
        hidden_copy(n - 1).start()

    for copy in lines:
        copy.wait_send()
    for copy in started:
        copy.wait_send()

    for step in range(1, n):
        source = lax.rem(me + step, n)
        send(
            hidden_out.at[source],
            hidden_in.at[source],
            h_s.at[source],
            h_r.at[source],
            source,
            core,
        ).wait()
    load_down.wait()
    hidden = jnp.transpose(hidden_in[...].reshape(n * cols, rows))
    chunk = 512

    def descend(step, carry):
        at = pl.ds(pl.multiple_of(step * chunk, chunk), chunk)
        sums_out[:, at] = jnp.dot(
            hidden, down_ref[:, at], preferred_element_type=jnp.float32
        ).astype(BF)
        return carry

    lax.fori_loop(0, width // chunk, descend, 0)
    swap = send(sums_out, sums_in, pair_s.at[3], pair_r.at[3], me, 1 - core)
    swap.start()
    swap.wait()
    pre = ALPHA * first_ref[...].reshape(rows, width).astype(jnp.float32) + (
        sums_out[...].astype(jnp.float32) + sums_in[...].astype(jnp.float32)
    )
    center = jnp.mean(pre, axis=1, keepdims=True)
    shifted = pre - center
    spread = jnp.mean(shifted * shifted, axis=1, keepdims=True)
    pre_ref[...] = shifted * lax.rsqrt(spread + EPS_NORM)
    half = pre_ref[:, pl.ds(pl.multiple_of(core * columns, columns), columns)]
    out_ref[...] = (half * gain2_ref[...]).astype(BF)


def spread(packed, weights, n):
    cols = weights.shape[1] // n
    rows = weights.shape[2]
    dma = pltpu.SemaphoreType.DMA
    return pl.pallas_call(
        functools.partial(spread_kernel, n),
        out_shape=(
            jax.ShapeDtypeStruct((n,) + packed.shape, BF),
            jax.ShapeDtypeStruct((2, cols, rows * n), BF),
        ),
        in_specs=[pl.BlockSpec(memory_space=pl.ANY)] * 2,
        out_specs=[pl.BlockSpec(memory_space=pl.ANY)] * 2,
        scratch_shapes=[dma((2,))] + [dma((n,))] * 6,
        compiler_params=pltpu.CompilerParams(collective_id=0, has_side_effects=True),
    )(packed, weights)


def feed(part, energy, resid, gain1, weights, taps, down, gain2, n):
    rows, columns = resid.shape
    width = part.shape[1]
    cols = weights.shape[0] // 2
    dma = pltpu.SemaphoreType.DMA
    vmem = pl.BlockSpec(memory_space=pltpu.VMEM)
    return pl.pallas_call(
        functools.partial(feed_kernel, n),
        out_shape=jax.ShapeDtypeStruct((rows, columns), BF),
        in_specs=[vmem] * 6 + [pl.BlockSpec(memory_space=pl.ANY), vmem],
        out_specs=vmem,
        scratch_shapes=[
            pltpu.VMEM(part.shape, BF),
            pltpu.VMEM(energy.shape, jnp.float32),
            pltpu.VMEM(resid.shape, BF),
            pltpu.VMEM((2, rows // 2, width), BF),
            pltpu.VMEM((n, 2, rows // 2, width), BF),
            pltpu.VMEM((n, 2 * cols, rows), BF),
            pltpu.VMEM((n, cols, rows), BF),
            pltpu.VMEM((n, cols, rows), BF),
            pltpu.VMEM(down.shape, BF),
            pltpu.VMEM((rows, width), BF),
            pltpu.VMEM((rows, width), BF),
            pltpu.VMEM((rows, width), jnp.float32),
            dma,
            dma((4,)),
            dma((4,)),
        ]
        + [dma((n // 4,))] * 10
        + [dma((n,))] * 4,
        compiler_params=pltpu.CompilerParams(
            collective_id=1, has_side_effects=True, vmem_limit_bytes=60000 * 1024
        ),
    )(part, energy, resid, gain1, weights, taps, down, gain2)


def pack(lat_n, k_rot):
    parts = [lat_n[:, at : at + LANES] for at in range(0, lat_n.shape[1], LANES)]
    whole = jnp.concatenate(parts + [k_rot.reshape(-1, LANES)], axis=0)
    return whole.reshape(2, whole.shape[0] // 2, LANES)


def unpack(lats, tok_rows, width):
    n = lats.shape[0]
    flat = lats.reshape(n, -1, LANES)
    split = tok_rows * (width // LANES)
    parts = [flat[:, at : at + tok_rows] for at in range(0, split, tok_rows)]
    return (
        jnp.concatenate(parts, axis=2).reshape(n * tok_rows, width),
        flat[:, split:].reshape(n * tok_rows, DR),
    )


def direct_fits(resid, latent, ffn_gate, n):
    return (
        lax.axis_size("tp") == 2
        and n % 4 == 0
        and resid.shape[0] == LANES
        and resid.shape[1] % LANES == 0
        and latent.shape[1] % LANES == 0
        and ffn_gate.shape[0] == LANES
        and ffn_gate.shape[1] % (16 * n) == 0
    )


def shards(
    resid,
    qa_nope,
    qb_nope,
    qa_rope,
    qb_rope,
    latent,
    key_rope,
    lat_gain,
    wa_key,
    wa_val,
    wb_key,
    wb_val,
    gain_a,
    gain_b,
    wa_out,
    wb_out,
    norm1_gain,
    ffn_gate,
    ffn_val,
    conv_gate,
    conv_val,
    ffn_down,
    norm2_gain,
):
    tok_rows = resid.shape[0]
    positions = lax.axis_index("sp") * tok_rows + jnp.arange(tok_rows)
    heads_a = qa_nope.shape[1] // DA
    heads_b = qb_nope.shape[1] // DB
    lat_n = rms_scale(latent, lat_gain).astype(jnp.bfloat16)
    k_rot = rotary(key_rope.astype(jnp.float32), positions).astype(jnp.bfloat16)
    rot_a = rotary(qa_rope.astype(jnp.float32).reshape(tok_rows, heads_a, DR), positions).astype(
        jnp.bfloat16
    )
    rot_b = rotary(qb_rope.astype(jnp.float32).reshape(tok_rows, heads_b, DR), positions).astype(
        jnp.bfloat16
    )
    query_a = qa_nope.reshape(tok_rows, heads_a, DA)
    query_b = qb_nope.reshape(tok_rows, heads_b, DB)

    def absorb(carry, query, q_rot, keys, k_part, vals):
        width = query.shape[2]
        scale = (width + DR) ** (-0.5)
        count = keys.shape[0]
        scores = jnp.einsum("qhd,khd->hqk", query, keys, preferred_element_type=jnp.float32)
        scores = (
            scores + jnp.einsum("qhr,kr->hqk", q_rot, k_part, preferred_element_type=jnp.float32)
        ) * scale
        key_pos = jnp.arange(count)
        allowed = key_pos[None, :] <= positions[:, None]
        scores = jnp.where(allowed[None], scores, -1e30)
        top_old, total_old, running_old = carry
        top_new = jnp.maximum(top_old, jnp.max(scores, axis=-1))
        weights = jnp.exp(scores - top_new[:, :, None])
        total_new = jnp.sum(weights, axis=-1)
        update = jnp.einsum(
            "hqk,khd->qhd", weights.astype(jnp.bfloat16), vals, preferred_element_type=jnp.float32
        )
        return (top_new, total_new, update)

    def project(source, weight, heads, width):
        result = jnp.dot(source, weight, preferred_element_type=jnp.float32).astype(jnp.bfloat16)
        return result.reshape(source.shape[0], heads, width)

    n = lax.axis_size("sp")
    fast = direct_fits(resid, latent, ffn_gate, n)
    if fast:
        stacked = jnp.stack([ffn_gate.T, ffn_val.T])
        lats, weights = spread(pack(lat_n, k_rot), stacked, n)
    empty = (start_carry(tok_rows, heads_a, DA), start_carry(tok_rows, heads_b, DB))
    if fast:
        pieces = unpack(lats, tok_rows, latent.shape[1])
    else:
        pieces = (
            lax.all_gather(lat_n, "sp", axis=0, tiled=True),
            lax.all_gather(k_rot, "sp", axis=0, tiled=True),
        )
    first_group = absorb(
        empty[0],
        query_a,
        rot_a,
        project(pieces[0], wa_key, heads_a, DA),
        pieces[1],
        project(pieces[0], wa_val, heads_a, DA),
    )
    second_group = absorb(
        empty[1],
        query_b,
        rot_b,
        project(pieces[0], wb_key, heads_b, DB),
        pieces[1],
        project(pieces[0], wb_val, heads_b, DB),
    )
    raw_a = divide_total(first_group)
    raw_b = divide_total(second_group)
    local_energy = jnp.sum(raw_a * raw_a, axis=1) + jnp.sum(raw_b * raw_b, axis=1)
    if fast:
        part = jnp.dot(
            (raw_a * gain_a).astype(BF), wa_out, preferred_element_type=jnp.float32
        ) + jnp.dot((raw_b * gain_b).astype(BF), wb_out, preferred_element_type=jnp.float32)
        cols = ffn_gate.shape[1] // n
        start = lax.axis_index("sp") * cols
        taps = jnp.concatenate(
            [lax.dynamic_slice_in_dim(taps, start, cols, 1).T for taps in (conv_gate, conv_val)]
        )
        return feed(
            part.astype(BF),
            jnp.broadcast_to(local_energy[:, None], (tok_rows, LANES)),
            resid,
            norm1_gain[None],
            weights.reshape(2 * cols, -1),
            taps,
            ffn_down,
            norm2_gain[None],
            n,
        )
    energy = lax.psum(local_energy, "tp")
    head_factor = lax.rsqrt(energy / (HA * DA + HB * DB) + EPS_RMS)[:, None]
    out_a = (raw_a * head_factor * gain_a).astype(jnp.bfloat16)
    out_b = (raw_b * head_factor * gain_b).astype(jnp.bfloat16)
    partial_value = jnp.dot(out_a, wa_out, preferred_element_type=jnp.float32) + jnp.dot(
        out_b, wb_out, preferred_element_type=jnp.float32
    )
    columns = resid.shape[1]
    mix_cols = lax.psum_scatter(
        partial_value.astype(jnp.bfloat16), "tp", scatter_dimension=1, tiled=True
    ).astype(jnp.float32)
    pre_one = ALPHA * resid.astype(jnp.float32) + mix_cols
    sums_one = lax.psum((jnp.sum(pre_one, axis=1), jnp.sum(pre_one * pre_one, axis=1)), "tp")
    gain_cols = lax.dynamic_slice_in_dim(norm1_gain, lax.axis_index("tp") * columns, columns, 0)
    first_cols = finish_norm(pre_one, sums_one, gain_cols, D).astype(jnp.bfloat16)
    first_full = lax.all_gather(first_cols, "tp", axis=1, tiled=True)
    pieces = (
        lax.all_gather(ffn_gate, "sp", axis=0, tiled=True),
        lax.all_gather(ffn_val, "sp", axis=0, tiled=True),
    )
    count = pieces[0].shape[0]
    gate_sum = jnp.dot(first_full, pieces[0], preferred_element_type=jnp.float32)
    val_sum = jnp.dot(first_full, pieces[1], preferred_element_type=jnp.float32)
    gate_up = gate_sum.astype(jnp.bfloat16)
    val_up = val_sum.astype(jnp.bfloat16)
    rim_gate, rim_val = passed_along(
        (gate_up[tok_rows - (KC - 1) :], val_up[tok_rows - (KC - 1) :]), "sp", 1
    )
    gate_c = causal_taps(jnp.concatenate([rim_gate, gate_up], axis=0), conv_gate, tok_rows)
    val_c = causal_taps(jnp.concatenate([rim_val, val_up], axis=0), conv_val, tok_rows)
    hidden = (jax.nn.silu(gate_c) * val_c).astype(jnp.bfloat16)
    down = jnp.dot(hidden, ffn_down, preferred_element_type=jnp.float32)
    ff_cols = lax.psum_scatter(
        down.astype(jnp.bfloat16), "tp", scatter_dimension=1, tiled=True
    ).astype(jnp.float32)
    pre_two = ALPHA * first_cols.astype(jnp.float32) + ff_cols
    sums_two = lax.psum((jnp.sum(pre_two, axis=1), jnp.sum(pre_two * pre_two, axis=1)), "tp")
    return finish_norm(pre_two, sums_two, norm2_gain, D).astype(jnp.bfloat16)


def solution(mesh):
    return jax.shard_map(
        shards,
        mesh=mesh,
        in_specs=(
            P("sp", "tp"),
            P("sp", "tp"),
            P("sp", "tp"),
            P("sp", "tp"),
            P("sp", "tp"),
            P("sp", None),
            P("sp", None),
            P(),
            P(None, "tp"),
            P(None, "tp"),
            P(None, "tp"),
            P(None, "tp"),
            P("tp"),
            P("tp"),
            P("tp", None),
            P("tp", None),
            P(),
            P("sp", "tp"),
            P("sp", "tp"),
            P(None, "tp"),
            P(None, "tp"),
            P("tp", None),
            P("tp"),
        ),
        out_specs=P("sp", "tp"),
        check_vma=False,
    )
```

```python
import functools

import jax
import jax.numpy as jnp
from jax import lax
from jax.experimental import pallas as pl
from jax.experimental.pallas import tpu as pltpu
from jax.sharding import PartitionSpec as P

D = 2048
HA = 16
DA = 64
HB = 8
DB = 128
DR = 32
KC = 3


THETA = 10000.0
EPS_RMS = 1e-06
EPS_NORM = 1e-05
ALPHA = 2.0**0.25


def passed_along(value, axis, steps):
    count = lax.axis_size(axis)
    leading, last = (max(0, -steps), min(count, count - steps))
    return lax.ppermute(value, axis, [(source, source + steps) for source in range(leading, last)])


def rotary(values, positions):
    half = values.shape[-1] // 2
    freq = THETA ** (-jnp.arange(half, dtype=jnp.float32) * 2.0 / values.shape[-1])
    angle = positions.astype(jnp.float32)[:, None] * freq[None, :]
    if values.ndim == 3:
        angle = angle[:, None, :]
    cosine = jnp.cos(angle)
    sine = jnp.sin(angle)
    first = values[..., :half]
    second = values[..., half:]
    return jnp.concatenate(
        [first * cosine - second * sine, second * cosine + first * sine], axis=-1
    )


def rms_scale(values, gain):
    wide = values.astype(jnp.float32)
    return wide * lax.rsqrt(jnp.mean(wide * wide, axis=-1, keepdims=True) + EPS_RMS) * gain


def finish_norm(values, sums, gain, width):
    center = sums[0] / width
    spread = sums[1] / width - center * center
    return (values - center[:, None]) * lax.rsqrt(spread + EPS_NORM)[:, None] * gain


def start_carry(count, heads, width):
    return (
        jnp.full((heads, count), -1e30, jnp.float32),
        jnp.zeros((heads, count), jnp.float32),
        jnp.zeros((count, heads, width), jnp.float32),
    )


def divide_total(carry):
    mixed = carry[2] / jnp.transpose(carry[1])[:, :, None]
    return mixed.reshape(mixed.shape[0], mixed.shape[1] * mixed.shape[2])


def causal_taps(extended, taps, count):
    total = jnp.zeros((count, extended.shape[1]), jnp.float32)
    for tap in range(KC):
        total = total + taps[tap] * extended[tap : tap + count].astype(jnp.float32)
    return total


BF = jnp.bfloat16
BF = jnp.bfloat16
LANES = 128
MESH = pl.DeviceIdType.MESH


def greet(n, tp):
    me, core = lax.axis_index("sp"), lax.axis_index("tp")
    barrier = pltpu.get_barrier_semaphore()
    for step in range(1, n):
        pl.semaphore_signal(
            barrier, inc=1, device_id=(lax.rem(me + step, n), core), device_id_type=MESH
        )
    pl.semaphore_signal(barrier, inc=1, device_id=(me, 1 - core), device_id_type=MESH)
    pl.semaphore_wait(barrier, n)


def send(src, dst, send_sem, recv_sem, sp, core):
    return pltpu.make_async_remote_copy(
        src_ref=src,
        dst_ref=dst,
        send_sem=send_sem,
        recv_sem=recv_sem,
        device_id=(sp, core),
        device_id_type=MESH,
    )


def block_order(n, me):
    depth = n // 4
    zi = me // 4
    if depth == 4:
        order = [zi, zi + 1 - 2 * lax.rem(zi, 2), 3 - zi, lax.rem(zi + 2, 4)]
        return order, order
    order = [lax.rem(zi + d, depth) for d in range(depth)]
    return order, [lax.rem(zi + depth - d, depth) for d in range(depth)]


class Gather:
    def __init__(self, n, own, full, sems):
        self.me, self.core = lax.axis_index("sp"), lax.axis_index("tp")
        me = self.me
        self.depth = n // 4
        self.own, self.full, self.sems = own, full, sems
        xi, yi = lax.rem(me, 2), lax.rem(me // 2, 2)
        self.x_peer, self.y_peer = me + 1 - 2 * xi, me + 2 - 4 * yi
        self.offs = [lax.rem(me, 4), lax.rem(self.x_peer, 4), lax.rem(self.y_peer, 4)]
        self.offs.append(3 - self.offs[0])
        self.order, self.targets = block_order(n, me)
        half = full.shape[2]
        cut = (half // 2 + 15) // 16 * 16
        self.cuts = (pl.ds(0, cut), pl.ds(cut, half - cut))
        self.started = []
        self.lines = [
            send(
                own.at[self.core],
                full.at[me, self.core],
                sems[0].at[d],
                sems[1].at[d],
                self.targets[d] * 4 + self.offs[0],
                self.core,
            )
            for d in range(1, self.depth)
        ]

    def block(self, d, place):
        return self.order[d] * 4 + self.offs[place]

    def share(self, d, place):
        block = self.block(d, place)
        ref = self.full.at[block, self.core]
        pair = self.sems[10], self.sems[11]
        return send(ref, ref, pair[0].at[block], pair[1].at[block], self.me, 1 - self.core)

    def across(self, d, x_way):
        ref = self.full.at[self.block(d, 0), self.core]
        src = self.own.at[self.core] if d == 0 else ref
        at = 2 if x_way else 4
        peer = self.x_peer if x_way else self.y_peer
        return send(src, ref, self.sems[at].at[d], self.sems[at + 1].at[d], peer, self.core)

    def corner(self, d, x_way):
        block = self.block(d, 2 if x_way else 1)
        ref = self.full.at[block, self.core, self.cuts[0 if x_way else 1]]
        at = 6 if x_way else 8
        peer = self.x_peer if x_way else self.y_peer
        return send(ref, ref, self.sems[at].at[d], self.sems[at + 1].at[d], peer, self.core)

    def go(self, copy):
        copy.start()
        self.started.append(copy)

    def stage_a(self, d):
        if d > 0:
            self.lines[d - 1].wait_recv()
        self.go(self.across(d, True))
        self.go(self.across(d, False))
        if d == 0:
            for copy in self.lines:
                copy.start()
        else:
            self.go(self.share(d, 0))

    def stage_b(self, d):
        self.across(d, True).wait_recv()
        self.go(self.corner(d, False))
        self.go(self.share(d, 1))
        self.across(d, False).wait_recv()
        self.go(self.corner(d, True))
        self.go(self.share(d, 2))

    def stage_c(self, d):
        self.corner(d, True).wait_recv()
        self.corner(d, False).wait_recv()
        self.go(self.share(d, 3))

    def arrived(self, d):
        for place in range(4):
            if d or place:
                self.share(d, place).wait_recv()

    def run(self, use, before=None):
        stages = ((self.stage_a, 0), (self.stage_b, 1), (self.stage_c, 2), (use, 3))
        for tick in range(self.depth + 3):
            for stage, lag in stages:
                if 0 <= tick - lag < self.depth:
                    stage(tick - lag)
            if tick == 0 and before is not None:
                before()

    def finish(self):
        for copy in self.lines + self.started:
            copy.wait_send()


def layer_kernel(
    n,
    lat_ref,
    qa_ref,
    qb_ref,
    ra_ref,
    rb_ref,
    cos_ref,
    sin_ref,
    wak_ref,
    wav_ref,
    wbk_ref,
    wbv_ref,
    gain_a_ref,
    gain_b_ref,
    resid_ref,
    gain1_ref,
    taps_ref,
    gain2_ref,
    out_a_hbm,
    out_b_hbm,
    down_hbm,
    columns_hbm,
    out_ref,
    lats,
    kk,
    att_a,
    att_b,
    out_a_w,
    out_b_w,
    weight_ref,
    part_ref,
    part_in,
    energy_ref,
    energy_in,
    resid_in,
    first_ref,
    full,
    ups,
    hidden_out,
    hidden_in,
    down_ref,
    sums_out,
    sums_in,
    pre_ref,
    load_sem,
    pair_s,
    pair_r,
    w_s,
    w_r,
    h_s,
    h_r,
    *gather_sems,
):
    me, core = lax.axis_index("sp"), lax.axis_index("tp")
    rows, columns = resid_ref.shape
    half_rows = rows // 2
    width = part_ref.shape[1]
    cols = hidden_in.shape[1]

    def piece(chip):
        return columns_hbm.at[:, pl.ds(pl.multiple_of(chip * cols, 16), cols), :]

    place = weight_ref.at[:, :, pl.ds(pl.multiple_of(me * rows, rows), rows)]
    own_w = pltpu.make_async_copy(piece(me), place, load_sem.at[0])
    loads = [
        own_w,
        pltpu.make_async_copy(out_a_hbm, out_a_w, load_sem.at[1]),
        pltpu.make_async_copy(out_b_hbm, out_b_w, load_sem.at[2]),
        pltpu.make_async_copy(down_hbm, down_ref, load_sem.at[3]),
    ]
    for copy in loads:
        copy.start()
    lats[me] = lat_ref[...]
    greet(n, 2)
    swap_resid = send(resid_ref, resid_in, pair_s.at[2], pair_r.at[2], me, 1 - core)
    w_copies = []
    for step in range(1, n):
        to = lax.rem(me + step, n)
        w_copies.append(send(piece(to), place, w_s.at[step], w_r.at[step], to, core))

    def behind_latents():
        swap_resid.start()

    lat_gather = Gather(n, lat_ref, lats, gather_sems[:12])

    def nothing(d):
        lat_gather.arrived(d)

    lat_gather.run(nothing, behind_latents)
    for copy in w_copies:
        copy.start()

    splits = (lats.shape[1] * lats.shape[2] - rows * DR // LANES) // rows
    lat_width = splits * LANES
    groups = LANES // DR
    group_rows = rows // groups
    into = lax.broadcasted_iota(jnp.int32, (LANES, LANES), 0)
    lane = lax.broadcasted_iota(jnp.int32, (LANES, LANES), 1)

    def lay_out(block, carry):
        flat = lats[block].reshape(-1, LANES)
        for at in range(splits):
            kk[block, :, at * LANES : (at + 1) * LANES] = flat[at * rows : (at + 1) * rows]
        packed = flat[splits * rows :]
        for group in range(groups):
            pick = (into == group * DR + lax.rem(lane, DR)).astype(jnp.float32).astype(BF)
            kk[block, group * group_rows : (group + 1) * group_rows, lat_width:] = jnp.dot(
                packed, pick, preferred_element_type=jnp.float32
            ).astype(BF)
        return carry

    lax.fori_loop(0, n, lay_out, 0)

    total_keys = n * rows
    q_pos = me * rows + lax.broadcasted_iota(jnp.int32, (rows, total_keys), 0)
    k_pos = lax.broadcasted_iota(jnp.int32, (rows, total_keys), 1)
    tile_lane = lax.broadcasted_iota(jnp.int32, (rows, LANES), 1)

    def head(h, q_ref, rot_ref, key_ref, val_ref, size, acc):
        scale = (size + DR) ** (-0.5)
        of_head = lax.broadcasted_iota(jnp.int32, q_ref.shape, 1) // size == h
        query = jnp.where(of_head, q_ref[...].astype(jnp.float32), 0.0).astype(BF)
        absorbed = lax.dot_general(
            query, key_ref[...], (((1,), (1,)), ((), ())), preferred_element_type=jnp.float32
        ).astype(BF)
        tile = rot_ref[:, pl.ds(pl.multiple_of((h // groups) * LANES, LANES), LANES)]
        tile = tile.astype(jnp.float32)
        swapped = jnp.where(
            lax.rem(tile_lane, DR) < DR // 2,
            pltpu.roll(tile, LANES - DR // 2, 1),
            pltpu.roll(tile, DR // 2, 1),
        )
        turned = tile * cos_ref[...] + swapped * sin_ref[...]
        turned = jnp.where(tile_lane // DR == lax.rem(h, groups), turned, 0.0).astype(BF)
        both = jnp.concatenate([absorbed, turned], axis=1)
        keys = kk[...].reshape(total_keys, lat_width + LANES)
        scores = (
            lax.dot_general(
                both, keys, (((1,), (1,)), ((), ())), preferred_element_type=jnp.float32
            )
            * scale
        )
        scores = jnp.where(k_pos <= q_pos, scores, -1e30)
        weights = jnp.exp(scores - jnp.max(scores, axis=1, keepdims=True))
        total = jnp.sum(weights, axis=1, keepdims=True)
        mixed = jnp.dot(
            weights.astype(BF), keys[:, :lat_width], preferred_element_type=jnp.float32
        )
        values = jnp.dot(
            (mixed / total).astype(BF), val_ref[...], preferred_element_type=jnp.float32
        )
        acc[...] = jnp.where(of_head, values, acc[...])

    def heads_a(h, carry):
        head(h, qa_ref, ra_ref, wak_ref, wav_ref, DA, att_a)
        return carry

    def heads_b(h, carry):
        head(h, qb_ref, rb_ref, wbk_ref, wbv_ref, DB, att_b)
        return carry

    att_a[...] = jnp.zeros_like(att_a)
    att_b[...] = jnp.zeros_like(att_b)
    lax.fori_loop(0, qa_ref.shape[1] // DA, heads_a, 0)
    lax.fori_loop(0, qb_ref.shape[1] // DB, heads_b, 0)
    raw_a, raw_b = att_a[...], att_b[...]
    local = jnp.sum(raw_a * raw_a, axis=1, keepdims=True)
    local = local + jnp.sum(raw_b * raw_b, axis=1, keepdims=True)
    energy_ref[...] = jnp.broadcast_to(local, energy_ref.shape)
    give_a = (raw_a * gain_a_ref[...]).astype(BF)
    give_b = (raw_b * gain_b_ref[...]).astype(BF)
    loads[1].wait()
    loads[2].wait()
    part_ref[...] = (
        jnp.dot(give_a, out_a_w[...], preferred_element_type=jnp.float32)
        + jnp.dot(give_b, out_b_w[...], preferred_element_type=jnp.float32)
    ).astype(BF)
    pair = [
        send(part_ref, part_in, pair_s.at[0], pair_r.at[0], me, 1 - core),
        send(energy_ref, energy_in, pair_s.at[1], pair_r.at[1], me, 1 - core),
    ]
    for copy in pair:
        copy.start()
    for copy in pair:
        copy.wait()
    swap_resid.wait()
    low = (core == 0).astype(jnp.float32)
    mine = resid_ref[...].astype(jnp.float32)
    other = resid_in[...].astype(jnp.float32)
    resid = jnp.concatenate(
        [mine * low + other * (1.0 - low), other * low + mine * (1.0 - low)], axis=1
    )
    energy = (energy_ref[...] + energy_in[...])[:, :1]
    factor = lax.rsqrt(energy / (HA * DA + HB * DB) + EPS_RMS)
    mix = (part_ref[...].astype(jnp.float32) + part_in[...].astype(jnp.float32)) * factor
    pre = ALPHA * resid + mix
    shifted = pre - jnp.mean(pre, axis=1, keepdims=True)
    spread = jnp.mean(shifted * shifted, axis=1, keepdims=True)
    first = (shifted * lax.rsqrt(spread + EPS_NORM) * gain1_ref[...]).astype(BF)
    first_ref[...] = first.reshape(2, half_rows, width)
    full[me] = first.reshape(2, half_rows, width)

    gather = Gather(n, first_ref, full, gather_sems[12:])

    def project_up(d):
        gather.arrived(d)
        if d == 0:
            for copy in w_copies:
                copy.wait()
            own_w.wait()
        base = gather.order[d] * 4

        def one(step, carry):
            block = base + step
            up = lax.dot_general(
                weight_ref[...].reshape(2 * cols, width),
                full[block].reshape(rows, width),
                (((1,), (1,)), ((), ())),
                preferred_element_type=jnp.float32,
            )
            ups[block] = up.astype(BF)
            return carry

        lax.fori_loop(0, 4, one, 0)

    gather.run(project_up)

    lane = lax.broadcasted_iota(jnp.int32, (2 * cols, rows), 1)

    def hidden_copy(block):
        return send(
            hidden_out.at[block], hidden_in.at[me], h_s.at[block], h_r.at[me], block, core
        )

    def convolve(block, before):
        current = ups[block].astype(jnp.float32)
        total = taps_ref[:, KC - 1 : KC] * current
        for back in range(1, KC):
            moved = jnp.where(
                lane < back, pltpu.roll(before, back, 1), pltpu.roll(current, back, 1)
            )
            total = total + taps_ref[:, KC - 1 - back : KC - back] * moved
        gate, val = total[:cols], total[cols:]
        hidden = gate / (1.0 + jnp.exp(-gate)) * val
        hidden_out[block] = hidden.astype(BF)

        @pl.when(block == me)
        def _():
            hidden_in[block] = hidden.astype(BF)

        @pl.when((block > 0) & (block - 1 != me))
        def _():
            hidden_copy(block - 1).start()

        return current

    lax.fori_loop(0, n, convolve, jnp.zeros((2 * cols, rows), jnp.float32))

    @pl.when(me != n - 1)
    def _():
        hidden_copy(n - 1).start()

    gather.finish()
    lat_gather.finish()

    for step in range(1, n):
        source = lax.rem(me + step, n)
        send(
            hidden_out.at[source],
            hidden_in.at[source],
            h_s.at[source],
            h_r.at[source],
            source,
            core,
        ).wait()
    loads[3].wait()
    hidden = jnp.transpose(hidden_in[...].reshape(n * cols, rows))
    chunk = 512

    def descend(step, carry):
        at = pl.ds(pl.multiple_of(step * chunk, chunk), chunk)
        sums_out[:, at] = jnp.dot(
            hidden, down_ref[:, at], preferred_element_type=jnp.float32
        ).astype(BF)
        return carry

    lax.fori_loop(0, width // chunk, descend, 0)
    swap = send(sums_out, sums_in, pair_s.at[3], pair_r.at[3], me, 1 - core)
    swap.start()
    swap.wait()
    pre = ALPHA * first_ref[...].reshape(rows, width).astype(jnp.float32) + (
        sums_out[...].astype(jnp.float32) + sums_in[...].astype(jnp.float32)
    )
    center = jnp.mean(pre, axis=1, keepdims=True)
    shifted = pre - center
    spread = jnp.mean(shifted * shifted, axis=1, keepdims=True)
    pre_ref[...] = shifted * lax.rsqrt(spread + EPS_NORM)
    half = pre_ref[:, pl.ds(pl.multiple_of(core * columns, columns), columns)]
    out_ref[...] = (half * gain2_ref[...]).astype(BF)


def layer(n, small, large, resid, latents, width, sizes):
    rows, columns = resid.shape
    lat_width, cols, down = sizes
    dma = pltpu.SemaphoreType.DMA
    vmem = pl.BlockSpec(memory_space=pltpu.VMEM)
    anywhere = pl.BlockSpec(memory_space=pl.ANY)
    heads = large[0].shape[0]
    gather_sems = [dma((n // 4,))] * 10 + [dma((n,))] * 2
    return pl.pallas_call(
        functools.partial(layer_kernel, n),
        out_shape=jax.ShapeDtypeStruct((rows, columns), BF),
        in_specs=[vmem] * len(small) + [anywhere] * len(large),
        out_specs=vmem,
        scratch_shapes=[
            pltpu.VMEM((n,) + latents, BF),
            pltpu.VMEM((n, rows, lat_width + LANES), BF),
            pltpu.VMEM((rows, large[0].shape[0]), jnp.float32),
            pltpu.VMEM((rows, large[1].shape[0]), jnp.float32),
            pltpu.VMEM(large[0].shape, BF),
            pltpu.VMEM(large[1].shape, BF),
            pltpu.VMEM((2, cols, width), BF),
            pltpu.VMEM((rows, width), BF),
            pltpu.VMEM((rows, width), BF),
            pltpu.VMEM((rows, LANES), jnp.float32),
            pltpu.VMEM((rows, LANES), jnp.float32),
            pltpu.VMEM(resid.shape, BF),
            pltpu.VMEM((2, rows // 2, width), BF),
            pltpu.VMEM((n, 2, rows // 2, width), BF),
            pltpu.VMEM((n, 2 * cols, rows), BF),
            pltpu.VMEM((n, cols, rows), BF),
            pltpu.VMEM((n, cols, rows), BF),
            pltpu.VMEM(down, BF),
            pltpu.VMEM((rows, width), BF),
            pltpu.VMEM((rows, width), BF),
            pltpu.VMEM((rows, width), jnp.float32),
            dma((4,)),
            dma((4,)),
            dma((4,)),
        ]
        + [dma((n,))] * 4
        + gather_sems * 2,
        compiler_params=pltpu.CompilerParams(
            collective_id=0, has_side_effects=True, vmem_limit_bytes=60 * 1024 * 1024
        ),
    )(*small, *large)


def pack(lat_n, k_rot):
    parts = [lat_n[:, at : at + LANES] for at in range(0, lat_n.shape[1], LANES)]
    groups = LANES // DR
    k_packed = k_rot.reshape(groups, -1, DR).transpose(1, 0, 2).reshape(-1, LANES)
    whole = jnp.concatenate(parts + [k_packed], axis=0)
    return whole.reshape(2, whole.shape[0] // 2, LANES)


def direct_fits(resid, latent, ffn_gate, n):
    return (
        lax.axis_size("tp") == 2
        and n % 4 == 0
        and resid.shape[0] == LANES
        and resid.shape[1] % LANES == 0
        and latent.shape[1] % LANES == 0
        and ffn_gate.shape[0] == LANES
        and ffn_gate.shape[1] % (16 * n) == 0
    )


def shards(
    resid,
    qa_nope,
    qb_nope,
    qa_rope,
    qb_rope,
    latent,
    key_rope,
    lat_gain,
    wa_key,
    wa_val,
    wb_key,
    wb_val,
    gain_a,
    gain_b,
    wa_out,
    wb_out,
    norm1_gain,
    ffn_gate,
    ffn_val,
    conv_gate,
    conv_val,
    ffn_down,
    norm2_gain,
):
    tok_rows = resid.shape[0]
    positions = lax.axis_index("sp") * tok_rows + jnp.arange(tok_rows)
    heads_a = qa_nope.shape[1] // DA
    heads_b = qb_nope.shape[1] // DB
    lat_n = rms_scale(latent, lat_gain).astype(jnp.bfloat16)
    k_rot = rotary(key_rope.astype(jnp.float32), positions).astype(jnp.bfloat16)
    n = lax.axis_size("sp")
    if direct_fits(resid, latent, ffn_gate, n):
        cols = ffn_gate.shape[1] // n
        start = lax.axis_index("sp") * cols
        taps = jnp.concatenate(
            [lax.dynamic_slice_in_dim(taps, start, cols, 1).T for taps in (conv_gate, conv_val)]
        )
        spot = jnp.arange(LANES) % DR
        freq = THETA ** (-(spot % (DR // 2)).astype(jnp.float32) * 2.0 / DR)
        angle = positions.astype(jnp.float32)[:, None] * freq[None, :]
        turn = jnp.where(spot < DR // 2, -1.0, 1.0)[None, :]
        packed = pack(lat_n, k_rot)
        small = (
            packed,
            qa_nope,
            qb_nope,
            qa_rope,
            qb_rope,
            jnp.cos(angle),
            jnp.sin(angle) * turn,
            wa_key,
            wa_val,
            wb_key,
            wb_val,
            gain_a[None],
            gain_b[None],
            resid,
            norm1_gain[None],
            taps,
            norm2_gain[None],
        )
        large = (wa_out, wb_out, ffn_down, jnp.stack([ffn_gate.T, ffn_val.T]))
        sizes = (latent.shape[1], cols, ffn_down.shape)
        return layer(n, small, large, resid, packed.shape, wa_out.shape[1], sizes)
    rot_a = rotary(qa_rope.astype(jnp.float32).reshape(tok_rows, heads_a, DR), positions).astype(
        jnp.bfloat16
    )
    rot_b = rotary(qb_rope.astype(jnp.float32).reshape(tok_rows, heads_b, DR), positions).astype(
        jnp.bfloat16
    )
    query_a = qa_nope.reshape(tok_rows, heads_a, DA)
    query_b = qb_nope.reshape(tok_rows, heads_b, DB)

    def absorb(carry, query, q_rot, keys, k_part, vals):
        width = query.shape[2]
        scale = (width + DR) ** (-0.5)
        count = keys.shape[0]
        scores = jnp.einsum("qhd,khd->hqk", query, keys, preferred_element_type=jnp.float32)
        scores = (
            scores + jnp.einsum("qhr,kr->hqk", q_rot, k_part, preferred_element_type=jnp.float32)
        ) * scale
        key_pos = jnp.arange(count)
        allowed = key_pos[None, :] <= positions[:, None]
        scores = jnp.where(allowed[None], scores, -1e30)
        top_old, total_old, running_old = carry
        top_new = jnp.maximum(top_old, jnp.max(scores, axis=-1))
        weights = jnp.exp(scores - top_new[:, :, None])
        total_new = jnp.sum(weights, axis=-1)
        update = jnp.einsum(
            "hqk,khd->qhd", weights.astype(jnp.bfloat16), vals, preferred_element_type=jnp.float32
        )
        return (top_new, total_new, update)

    def project(source, weight, heads, width):
        result = jnp.dot(source, weight, preferred_element_type=jnp.float32).astype(jnp.bfloat16)
        return result.reshape(source.shape[0], heads, width)

    empty = (start_carry(tok_rows, heads_a, DA), start_carry(tok_rows, heads_b, DB))
    pieces = (
        lax.all_gather(lat_n, "sp", axis=0, tiled=True),
        lax.all_gather(k_rot, "sp", axis=0, tiled=True),
    )
    first_group = absorb(
        empty[0],
        query_a,
        rot_a,
        project(pieces[0], wa_key, heads_a, DA),
        pieces[1],
        project(pieces[0], wa_val, heads_a, DA),
    )
    second_group = absorb(
        empty[1],
        query_b,
        rot_b,
        project(pieces[0], wb_key, heads_b, DB),
        pieces[1],
        project(pieces[0], wb_val, heads_b, DB),
    )
    raw_a = divide_total(first_group)
    raw_b = divide_total(second_group)
    local_energy = jnp.sum(raw_a * raw_a, axis=1) + jnp.sum(raw_b * raw_b, axis=1)
    energy = lax.psum(local_energy, "tp")
    head_factor = lax.rsqrt(energy / (HA * DA + HB * DB) + EPS_RMS)[:, None]
    out_a = (raw_a * head_factor * gain_a).astype(jnp.bfloat16)
    out_b = (raw_b * head_factor * gain_b).astype(jnp.bfloat16)
    partial_value = jnp.dot(out_a, wa_out, preferred_element_type=jnp.float32) + jnp.dot(
        out_b, wb_out, preferred_element_type=jnp.float32
    )
    columns = resid.shape[1]
    mix_cols = lax.psum_scatter(
        partial_value.astype(jnp.bfloat16), "tp", scatter_dimension=1, tiled=True
    ).astype(jnp.float32)
    pre_one = ALPHA * resid.astype(jnp.float32) + mix_cols
    sums_one = lax.psum((jnp.sum(pre_one, axis=1), jnp.sum(pre_one * pre_one, axis=1)), "tp")
    gain_cols = lax.dynamic_slice_in_dim(norm1_gain, lax.axis_index("tp") * columns, columns, 0)
    first_cols = finish_norm(pre_one, sums_one, gain_cols, D).astype(jnp.bfloat16)
    first_full = lax.all_gather(first_cols, "tp", axis=1, tiled=True)
    pieces = (
        lax.all_gather(ffn_gate, "sp", axis=0, tiled=True),
        lax.all_gather(ffn_val, "sp", axis=0, tiled=True),
    )
    count = pieces[0].shape[0]
    gate_sum = jnp.dot(first_full, pieces[0], preferred_element_type=jnp.float32)
    val_sum = jnp.dot(first_full, pieces[1], preferred_element_type=jnp.float32)
    gate_up = gate_sum.astype(jnp.bfloat16)
    val_up = val_sum.astype(jnp.bfloat16)
    rim_gate, rim_val = passed_along(
        (gate_up[tok_rows - (KC - 1) :], val_up[tok_rows - (KC - 1) :]), "sp", 1
    )
    gate_c = causal_taps(jnp.concatenate([rim_gate, gate_up], axis=0), conv_gate, tok_rows)
    val_c = causal_taps(jnp.concatenate([rim_val, val_up], axis=0), conv_val, tok_rows)
    hidden = (jax.nn.silu(gate_c) * val_c).astype(jnp.bfloat16)
    down = jnp.dot(hidden, ffn_down, preferred_element_type=jnp.float32)
    ff_cols = lax.psum_scatter(
        down.astype(jnp.bfloat16), "tp", scatter_dimension=1, tiled=True
    ).astype(jnp.float32)
    pre_two = ALPHA * first_cols.astype(jnp.float32) + ff_cols
    sums_two = lax.psum((jnp.sum(pre_two, axis=1), jnp.sum(pre_two * pre_two, axis=1)), "tp")
    return finish_norm(pre_two, sums_two, norm2_gain, D).astype(jnp.bfloat16)


def solution(mesh):
    return jax.shard_map(
        shards,
        mesh=mesh,
        in_specs=(
            P("sp", "tp"),
            P("sp", "tp"),
            P("sp", "tp"),
            P("sp", "tp"),
            P("sp", "tp"),
            P("sp", None),
            P("sp", None),
            P(),
            P(None, "tp"),
            P(None, "tp"),
            P(None, "tp"),
            P(None, "tp"),
            P("tp"),
            P("tp"),
            P("tp", None),
            P("tp", None),
            P(),
            P("sp", "tp"),
            P("sp", "tp"),
            P(None, "tp"),
            P(None, "tp"),
            P("tp", None),
            P("tp"),
        ),
        out_specs=P("sp", "tp"),
        check_vma=False,
    )
```
